32 devices in a mesh: fs: 16 (over z, y, x), tp: 2 (over core).
Axes of the slice: x: 2, y: 2, z: 4, core: 2. Of those that a mesh axis runs over, the one named last changes fastest.
Arguments:
- layer_input: bfloat16 [16384, 2048], P('fs'), may hold values from -6 to 6
- value_cotangent: bfloat16 [16384, 1024], P('fs', 'tp'), may hold values from -0.046875 to 0.046875
- mixed_output: bfloat16 [16384, 1024], P('fs'), may hold values from -6 to 6
- output_cotangent: bfloat16 [16384, 2048], P('fs', 'tp'), may hold values from -0.046875 to 0.046875
- value_weight: float32 [2048, 1024], P('fs', 'tp'), may hold values from -0.125 to 0.125
- out_weight: float32 [1024, 2048], P('fs', 'tp'), may hold values from -0.1875 to 0.1875
- value_basis: bfloat16 [2048, 256], P('fs'), may hold values from -0.125 to 0.125
- out_basis: bfloat16 [1024, 256], P('fs'), may hold values from -0.1875 to 0.1875
- value_first: float32 [256, 1024], P('fs', 'tp'), may hold values from -6 to 6
- value_second: float32 [256, 1024], P('fs', 'tp'), may hold values from 0.5 to 2
- out_first: float32 [256, 2048], P('fs', 'tp'), may hold values from -6 to 6
- out_second: float32 [256, 2048], P('fs', 'tp'), may hold values from 0.5 to 2
Outputs:
- value_new: float32 [2048, 1024], P('fs', 'tp')
- out_new: float32 [1024, 2048], P('fs', 'tp')
- value_step: float32 [2048, 1024], P('fs', 'tp')
- out_step: float32 [1024, 2048], P('fs', 'tp')
- value_copy: bfloat16 [2048, 1024], P(None, 'tp')
- out_copy: bfloat16 [1024, 2048], P(None, 'tp')
- value_first_new: float32 [256, 1024], P('fs', 'tp')
- value_second_new: float32 [256, 1024], P('fs', 'tp')
- out_first_new: float32 [256, 2048], P('fs', 'tp')
- out_second_new: float32 [256, 2048], P('fs', 'tp')
The draws below stay inside these ranges and needn't reach their ends.
All inputs are finite; a program needn't handle non-finite values.
Results may differ from the reference program's by a relative error of at most 0.00045.
Values may be sent and summed in bfloat16 or wider, within the bound.
A program may use at most 64 MiB of HBM per device.

```python
import math
import jax
import jax.numpy as jnp
from jax import lax

D = 2048
W = 1024
R = 256
TOKENS = 16384


def levels(stream_key, dims, cuts, low, largest):
    gain = 1.0
    for axis_at, shards_of in cuts:
        steps = jax.random.uniform(jax.random.fold_in(jax.random.fold_in(stream_key, 6), axis_at), (shards_of,), jnp.float32, low / len(cuts), largest / len(cuts))
        gain = gain * jnp.repeat(jnp.exp(steps), dims[axis_at] // shards_of).reshape((-1,) + (1,) * (len(dims) - 1 - axis_at))
    return gain


def noise(stream_key, shape, spread, reach, split=(), kind=jnp.bfloat16):
    entries = jax.random.normal(stream_key, shape, jnp.float32) * spread
    if len(split) > 0:
        entries = levels(stream_key, shape, split, -0.22, 0.18) * entries
    return jnp.clip(entries, min=-reach, max=reach).astype(kind)


def setup_inputs(seed: int = 0) -> dict:
    key_of = jax.random.split(jax.random.key(seed), 13)
    return {
        "layer_input": noise(key_of[0], (TOKENS, D), 1.0, 6.0, ((0, 16),)),
        "value_cotangent": noise(key_of[1], (TOKENS, W), (1.0 / TOKENS ** 0.5), 0.046875, ((0, 16), (1, 2))),
        "mixed_output": noise(key_of[2], (TOKENS, W), 1.0, 6.0, ((0, 16),)),
        "output_cotangent": noise(key_of[3], (TOKENS, D), (1.0 / TOKENS ** 0.5), 0.046875, ((0, 16), (1, 2))),
        "value_weight": noise(key_of[4], (D, W), D ** -0.5, 0.125, ((0, 16), (1, 2)), jnp.float32),
        "out_weight": noise(key_of[5], (W, D), W ** -0.5, 0.1875, ((0, 16), (1, 2)), jnp.float32),
        "value_basis": noise(key_of[6], (D, R), D ** -0.5, 0.125, ((0, 16),)),
        "out_basis": noise(key_of[7], (W, R), W ** -0.5, 0.1875, ((0, 16),)),
        "value_first": noise(key_of[8], (R, W), 1.0, 6.0, ((0, 16), (1, 2)), jnp.float32),
        "value_second": jnp.clip(jnp.exp(math.log(2.0) - 1.3862944 * jax.random.uniform(key_of[9], (R, W), jnp.float32) ** levels(key_of[9], (R, W), ((0, 16), (1, 2)), -0.2, 0.2)), 0.5, 2.0),
        "out_first": noise(key_of[10], (R, D), 1.0, 6.0, ((0, 16), (1, 2)), jnp.float32),
        "out_second": jnp.clip(jnp.exp(math.log(2.0) - 1.3862944 * jax.random.uniform(key_of[11], (R, D), jnp.float32) ** levels(key_of[11], (R, D), ((0, 16), (1, 2)), -0.2, 0.2)), 0.5, 2.0),
    }


first_decay = 0.8
second_decay = 0.9
step_rate = 0.1

def contract(left, right, precision=None):
    return lax.dot_general(left, right, (((0,), (0,)), ((), ())), preferred_element_type=jnp.float32, precision=precision)

def moments(projected, first, second):
    first_new = first_decay * first + (1.0 - first_decay) * projected
    second_new = second_decay * second + (1.0 - second_decay) * projected * projected
    return (first_new, second_new, first_new / jnp.sqrt(second_new))

def reference(layer_input, value_cotangent, mixed_output, output_cotangent, value_weight, out_weight, value_basis, out_basis, value_first, value_second, out_first, out_second):
    highest = lax.Precision.HIGHEST
    value_grad = contract(layer_input, value_cotangent)
    out_grad = contract(mixed_output, output_cotangent)
    value_proj = contract(value_basis.astype(jnp.float32), value_grad, highest)
    out_proj = contract(out_basis.astype(jnp.float32), out_grad, highest)
    value_first_new, value_second_new, value_dir = moments(value_proj, value_first, value_second)
    out_first_new, out_second_new, out_dir = moments(out_proj, out_first, out_second)
    total = jnp.sum(value_dir * value_dir) + jnp.sum(out_dir * out_dir)
    scale = step_rate / jnp.sqrt(1.0 + total / (R * (W + D)))
    value_step = scale * jnp.dot(value_basis.astype(jnp.float32), value_dir, precision=highest)
    out_step = scale * jnp.dot(out_basis.astype(jnp.float32), out_dir, precision=highest)
    value_new = value_weight - value_step
    out_new = out_weight - out_step
    return (value_new, out_new, value_step, out_step, value_new.astype(jnp.bfloat16), out_new.astype(jnp.bfloat16), value_first_new, value_second_new, out_first_new, out_second_new)
```

```python
import functools
import itertools

import jax
import jax.numpy as jnp
from jax import lax
from jax.experimental import pallas as pl
from jax.experimental.pallas import tpu as pltpu
from jax.sharding import PartitionSpec as P

first_decay = 0.8
second_decay = 0.9
step_rate = 0.1


def split_digits(n):
    digits = []
    stride = 1
    for _ in range(2):
        if n % 2 == 0 and n > 2:
            digits.append((2, stride))
            stride *= 2
            n //= 2
    digits.append((n, stride))
    return digits


def orders_of(digits):
    slow, fast = digits[-1], digits[:-1]
    return [slow, *fast], [slow, *fast[::-1]]


def shifted(me, order, offsets, sign):
    out = me
    for (size, stride), off in zip(order, offsets):
        if off:
            digit = lax.rem(lax.div(me, stride), size)
            other = lax.rem(digit + (off if sign > 0 else size - off), size)
            out = out + (other - digit) * stride
    return out


def flat(order, offsets):
    out = 0
    for (size, _), off in zip(order, offsets):
        out = out * size + off
    return out


class Gather:
    def __init__(self, me, dst, order, send_sem, recv_sem):
        self.me, self.dst, self.order = me, dst, order
        self.send_sem, self.recv_sem = send_sem, recv_sem
        self.sent = []

    def copy(self, held, axis, off):
        target = tuple(off if i == axis else h for i, h in enumerate(held))
        slot = flat(self.order, target)
        block = shifted(self.me, self.order, held, -1)
        peer = shifted(self.me, self.order, tuple(off if i == axis else 0 for i in range(len(held))), 1)
        return pltpu.make_async_remote_copy(
            src_ref=self.dst.at[block],
            dst_ref=self.dst.at[block],
            send_sem=self.send_sem.at[slot],
            recv_sem=self.recv_sem.at[slot],
            device_id={"fs": peer},
            device_id_type=pl.DeviceIdType.MESH,
        )

    def forward(self, held):
        last = max([i for i, h in enumerate(held) if h], default=-1)
        for axis in range(last + 1, len(self.order)):
            for off in range(1, self.order[axis][0]):
                c = self.copy(held, axis, off)
                c.start()
                self.sent.append(c)

    def arrive(self, held):
        if any(held):
            slot = flat(self.order, held)
            block = shifted(self.me, self.order, held, -1)
            pltpu.make_async_remote_copy(
                src_ref=self.dst.at[block],
                dst_ref=self.dst.at[block],
                send_sem=self.send_sem.at[slot],
                recv_sem=self.recv_sem.at[slot],
                device_id={"fs": self.me},
                device_id_type=pl.DeviceIdType.MESH,
            ).wait_recv()

    def all_held(self):
        rows = list(itertools.product(*[range(s) for s, _ in self.order]))
        return sorted(rows, key=lambda h: max([i for i, v in enumerate(h) if v], default=-1))

    def drain(self):
        for c in self.sent:
            c.wait_send()


def gather_all(gathers, started=()):
    for steps in itertools.zip_longest(*[g.all_held() for g in gathers]):
        for g, held in zip(gathers, steps):
            if held is not None:
                g.arrive(held)
                g.forward(held)
    for g in gathers:
        g.drain()


class Scatter:
    def __init__(self, me, part, bufs, stage, order, send_sem, recv_sem):
        self.me, self.part, self.bufs, self.stage = me, part, bufs, stage
        self.order, self.send_sem, self.recv_sem = order, send_sem, recv_sem
        self.sent = []

    def slot(self, js):
        return flat(self.order, js)

    def copy(self, js):
        axis = next(i for i, j in enumerate(js) if j)
        slot = self.slot(js)
        peer = shifted(self.me, self.order, tuple(j if i == axis else 0 for i, j in enumerate(js)), 1)
        src = self.part.at[shifted(self.me, self.order, js, 1)] if axis == 0 else self.stage.at[slot]
        return pltpu.make_async_remote_copy(
            src_ref=src,
            dst_ref=self.bufs.at[slot],
            send_sem=self.send_sem.at[slot],
            recv_sem=self.recv_sem.at[slot],
            device_id={"fs": peer},
            device_id_type=pl.DeviceIdType.MESH,
        )

    def summed(self, js):
        axis = next((i for i, j in enumerate(js) if j), len(js))
        total = self.part[shifted(self.me, self.order, js, 1)]
        for i in range(axis):
            for off in range(1, self.order[i][0]):
                src = tuple(off if k == i else (js[k] if k > i else 0) for k in range(len(js)))
                self.copy(src).wait_recv()
                total = total + self.bufs[self.slot(src)]
        return total

    def tasks(self):
        rows = list(itertools.product(*[range(s) for s, _ in self.order]))
        first = lambda js: next((i for i, j in enumerate(js) if j), len(js))
        return sorted(rows, key=lambda js: (first(js), first(js[first(js) + 1:]) if first(js) < len(js) else 0))

    def run(self, js):
        if not any(js):
            return
        axis = next(i for i, j in enumerate(js) if j)
        if axis > 0:
            self.stage[self.slot(js)] = self.summed(js)
        c = self.copy(js)
        c.start()
        self.sent.append(c)

    def drain(self):
        for c in self.sent:
            c.wait_send()


def two_parts(wide):
    upper = wide.astype(jnp.bfloat16)
    lower = (wide - upper.astype(jnp.float32)).astype(jnp.bfloat16)
    return upper, lower


def dot(a, b, dims=(((1,), (0,)), ((), ()))):
    return lax.dot_general(a, b, dims, preferred_element_type=jnp.float32)


def merged(ref):
    n, r, c = ref.shape
    if r % 8 == 0:
        return ref[...].reshape(n * r, c)
    return jnp.concatenate([ref[i] for i in range(n)], axis=0)


def kernel(
    n, m, total_size,
    x_hbm, vc_hbm, mo_hbm, oc_hbm,
    vw, ow, vb, ob, vf, vs, of, os_,
    vnew, onew, vstep, ostep, vcopy, ocopy, vf_new, vs_new, of_new, os_new,
    x_ref, vc_ref, mo_ref, oc_ref,
    vb_all, ob_all, vpart, opart, vacc, oacc, vrs, ors, vstage, ostage, vdir, odir, squares,
    load_sem, g_send, g_recv, s_send, s_recv, q_send, q_recv,
):
    me = lax.axis_index("fs")
    mine = lax.axis_index("tp")
    digits = split_digits(n)
    order_a, order_b = orders_of(digits)

    loads = [
        pltpu.make_async_copy(src, dst, load_sem.at[i])
        for i, (src, dst) in enumerate(((x_hbm, x_ref), (vc_hbm, vc_ref), (mo_hbm, mo_ref), (oc_hbm, oc_ref)))
    ]
    for c in loads:
        c.start()
    vb_all[me] = vb[...]
    ob_all[me] = ob[...]

    barrier = pltpu.get_barrier_semaphore()
    peers = 0
    for size, stride in digits:
        for off in range(1, size):
            pl.semaphore_signal(
                barrier, inc=1, device_id={"fs": shifted(me, [(size, stride)], (off,), 1)},
                device_id_type=pl.DeviceIdType.MESH,
            )
            peers += 1
    for off in range(1, m):
        pl.semaphore_signal(
            barrier, inc=1, device_id={"tp": lax.rem(mine + off, m)},
            device_id_type=pl.DeviceIdType.MESH,
        )
        peers += 1
    pl.semaphore_wait(barrier, peers)

    gather_all([
        Gather(me, vb_all, order_a, g_send.at[0], g_recv.at[0]),
        Gather(me, ob_all, order_b, g_send.at[1], g_recv.at[1]),
    ])
    for c in loads:
        c.wait()

    tokens = x_ref.shape[0]
    tile = min(256, tokens)
    v_basis = merged(vb_all)
    o_basis = merged(ob_all)
    vacc[...] = jnp.zeros_like(vacc)
    oacc[...] = jnp.zeros_like(oacc)

    def project(src, cot, basis, acc):
        def body(t, carry):
            rows = pl.ds(pl.multiple_of(t * tile, tile), tile)
            upper, lower = two_parts(dot(src[rows, :], basis))
            dims = (((0,), (0,)), ((), ()))
            cots = cot[rows, :]
            acc[...] += dot(upper, cots, dims) + dot(lower, cots, dims)
            return carry
        lax.fori_loop(0, tokens // tile, body, 0)

    project(mo_ref, oc_ref, o_basis, oacc)
    project(x_ref, vc_ref, v_basis, vacc)
    r = vpart.shape[1]
    for i in range(n):
        vpart[i] = vacc[i * r:(i + 1) * r, :]
        opart[i] = oacc[i * r:(i + 1) * r, :]

    scatters = [
        Scatter(me, vpart, vrs, vstage, order_a[::-1], s_send.at[0], s_recv.at[0]),
        Scatter(me, opart, ors, ostage, order_b[::-1], s_send.at[1], s_recv.at[1]),
    ]
    for steps in zip(*[s.tasks() for s in scatters]):
        for s, js in zip(scatters, steps):
            s.run(js)

    def moments(projected, first, second, first_new, second_new):
        fn = first_decay * first[...] + (1.0 - first_decay) * projected
        sn = second_decay * second[...] + (1.0 - second_decay) * projected * projected
        first_new[...] = fn
        second_new[...] = sn
        return fn / jnp.sqrt(sn)

    zero = (0,) * len(digits)
    vdir[me] = moments(scatters[0].summed(zero), vf, vs, vf_new, vs_new)
    odir[me] = moments(scatters[1].summed(zero), of, os_, of_new, os_new)
    for s in scatters:
        s.drain()

    gather_all([
        Gather(me, vdir, order_a, g_send.at[2], g_recv.at[2]),
        Gather(me, odir, order_b, g_send.at[3], g_recv.at[3]),
    ])
    v_dir = merged(vdir)
    o_dir = merged(odir)
    squares[0] = jnp.full(squares.shape[1:], jnp.sum(v_dir * v_dir) + jnp.sum(o_dir * o_dir), jnp.float32)
    traded = []
    for off in range(1, m):
        c = pltpu.make_async_remote_copy(
            src_ref=squares.at[0], dst_ref=squares.at[off],
            send_sem=q_send.at[off], recv_sem=q_recv.at[off],
            device_id={"tp": lax.rem(mine + off, m)}, device_id_type=pl.DeviceIdType.MESH,
        )
        c.start()
        traded.append(c)
    v_upper, v_lower = two_parts(v_dir)
    o_upper, o_lower = two_parts(o_dir)
    v_sum = dot(vb[...], v_upper) + dot(vb[...], v_lower)
    o_sum = dot(ob[...], o_upper) + dot(ob[...], o_lower)
    for c in traded:
        c.wait()
    total = squares[0]
    for off in range(1, m):
        total = total + squares[off]
    scale = (step_rate / jnp.sqrt(1.0 + total / total_size))[0:1, 0:1]

    def update(weight, product, new, step, copy):
        s = scale * product
        w = weight[...] - s
        step[...] = s
        new[...] = w
        copy[me] = w.astype(jnp.bfloat16)

    update(vw, v_sum, vnew, vstep, vcopy)
    update(ow, o_sum, onew, ostep, ocopy)

    gather_all([
        Gather(me, vcopy, order_a, g_send.at[4], g_recv.at[4]),
        Gather(me, ocopy, order_b, g_send.at[5], g_recv.at[5]),
    ])


def local(n, m, x, vc, mo, oc, vw, ow, vb, ob, vf, vs, of, os_):
    f32, bf16 = jnp.float32, jnp.bfloat16
    shape = jax.ShapeDtypeStruct
    r, v_cols = vf.shape
    o_cols = of.shape[1]
    total_size = float(n * r * m * (v_cols + o_cols))
    vmem = pl.BlockSpec(memory_space=pltpu.VMEM)
    hbm = pl.BlockSpec(memory_space=pl.ANY)
    outs = (
        shape(vw.shape, f32), shape(ow.shape, f32),
        shape(vw.shape, f32), shape(ow.shape, f32),
        shape((n, *vw.shape), bf16), shape((n, *ow.shape), bf16),
        shape(vf.shape, f32), shape(vf.shape, f32), shape(of.shape, f32), shape(of.shape, f32),
    )
    dma = pltpu.SemaphoreType.DMA
    res = pl.pallas_call(
        functools.partial(kernel, n, m, total_size),
        out_shape=outs,
        in_specs=[hbm] * 4 + [vmem] * 8,
        out_specs=[vmem] * 10,
        scratch_shapes=[
            pltpu.VMEM(x.shape, bf16), pltpu.VMEM(vc.shape, bf16),
            pltpu.VMEM(mo.shape, bf16), pltpu.VMEM(oc.shape, bf16),
            pltpu.VMEM((n, *vb.shape), bf16), pltpu.VMEM((n, *ob.shape), bf16),
            pltpu.VMEM((n, r, v_cols), f32), pltpu.VMEM((n, r, o_cols), f32),
            pltpu.VMEM((n * r, v_cols), f32), pltpu.VMEM((n * r, o_cols), f32),
            pltpu.VMEM((n, r, v_cols), f32), pltpu.VMEM((n, r, o_cols), f32),
            pltpu.VMEM((n, r, v_cols), f32), pltpu.VMEM((n, r, o_cols), f32),
            pltpu.VMEM((n, r, v_cols), f32), pltpu.VMEM((n, r, o_cols), f32),
            pltpu.VMEM((m, 8, 128), f32),
            dma((4,)), dma((6, n)), dma((6, n)), dma((2, n)), dma((2, n)), dma((m,)), dma((m,)),
        ],
        compiler_params=pltpu.CompilerParams(
            collective_id=0, has_side_effects=True, vmem_limit_bytes=60 * 1024 * 1024
        ),
    )(x, vc, mo, oc, vw, ow, vb, ob, vf, vs, of, os_)
    vcopy, ocopy = res[4], res[5]
    return (
        *res[:4],
        vcopy.reshape(n * vw.shape[0], v_cols),
        ocopy.reshape(n * ow.shape[0], o_cols),
        *res[6:],
    )


def solution(mesh):
    n, m = mesh.shape["fs"], mesh.shape["tp"]
    rows, both, cols = P("fs", None), P("fs", "tp"), P(None, "tp")
    return jax.shard_map(
        functools.partial(local, n, m),
        mesh=mesh,
        in_specs=(rows, both, rows, both, both, both, rows, rows, both, both, both, both),
        out_specs=(both, both, both, both, cols, cols, both, both, both, both),
        check_vma=False,
    )
```

```python
import functools
import itertools

import jax
import jax.numpy as jnp
from jax import lax
from jax.experimental import pallas as pl
from jax.experimental.pallas import tpu as pltpu
from jax.sharding import PartitionSpec as P

first_decay = 0.8
second_decay = 0.9
step_rate = 0.1


def split_digits(n):
    digits = []
    stride = 1
    for _ in range(2):
        if n % 2 == 0 and n > 2:
            digits.append((2, stride))
            stride *= 2
            n //= 2
    digits.append((n, stride))
    return digits


def orders_of(digits):
    slow, fast = digits[-1], digits[:-1]
    return [slow, *fast], [slow, *fast[::-1]]


def shifted(me, order, offsets, sign):
    out = me
    for (size, stride), off in zip(order, offsets):
        if off:
            digit = lax.rem(lax.div(me, stride), size)
            other = lax.rem(digit + (off if sign > 0 else size - off), size)
            out = out + (other - digit) * stride
    return out


def flat(order, offsets):
    out = 0
    for (size, _), off in zip(order, offsets):
        out = out * size + off
    return out


class Line:
    def __init__(self, me, digit):
        self.size, self.stride = digit
        self.me = me
        self.at = lax.div(me, self.stride)

    def nearest(self, t):
        if t == 0:
            return self.at
        k, z = self.size, self.at
        near = jnp.minimum(z, k - 1 - z)
        low = z < k - 1 - z
        step = (t + 1) // 2 if t % 2 else -(t // 2)
        both = jnp.where(low, z - step, z + step)
        one = jnp.where(low, z + (t - near), z - (t - near))
        return jnp.where(t <= 2 * near, both, one)


class Gather:
    def __init__(self, me, dst, order, send_sem, recv_sem):
        self.me, self.dst, self.order = me, dst, order
        self.line = Line(me, order[0])
        self.send_sem, self.recv_sem = send_sem, recv_sem
        self.sent = []

    def events(self):
        fast = list(itertools.product(*[range(s) for s, _ in self.order[1:]]))
        rows = []
        for t in range(self.order[0][0]):
            for js in fast:
                phase = max([i + 1 for i, j in enumerate(js) if j], default=0)
                due = t + 1.25 * phase if phase < len(self.order) - 1 else 100 + t
                rows.append((due, phase, t, js))
        return sorted(rows)

    def block(self, event):
        _, _, t, js = event
        z = self.line.nearest(t)
        return shifted(self.me, self.order[1:], js, -1) + (z - self.line.at) * self.line.stride

    def copy(self, block, peer, way):
        return pltpu.make_async_remote_copy(
            src_ref=self.dst(block),
            dst_ref=self.dst(block),
            send_sem=self.send_sem.at[block, way],
            recv_sem=self.recv_sem.at[block],
            device_id={"fs": peer},
            device_id_type=pl.DeviceIdType.MESH,
        )

    def start(self, cond, c):
        if cond is None:
            c.start()
        else:
            pl.when(cond)(c.start)
        self.sent.append((cond, c))

    def forward(self, event):
        _, phase, t, js = event
        block = self.block(event)
        if phase == 0:
            z, k, stride = self.line.at, self.line.size, self.line.stride
            source = self.line.nearest(t)
            up = z + 1 < k
            down = z > 0
            if t > 0:
                up = jnp.logical_and(up, source < z)
                down = jnp.logical_and(down, source > z)
            self.start(up, self.copy(block, jnp.minimum(self.me + stride, k * stride - stride + lax.rem(self.me, stride)), 0))
            self.start(down, self.copy(block, jnp.maximum(self.me - stride, lax.rem(self.me, stride)), 1))
        way = 2
        for axis in range(1, len(self.order)):
            size = self.order[axis][0]
            for off in range(1, size):
                if axis > phase:
                    peer = shifted(self.me, [self.order[axis]], (off,), 1)
                    self.start(None, self.copy(block, peer, way))
                way += 1

    def arrive(self, event):
        if event[2] or any(event[3]):
            self.copy(self.block(event), shifted(self.me, [self.order[-1]], (1,), 1), 0).wait_recv()

    def drain(self):
        for cond, c in self.sent:
            if cond is None:
                c.wait_send()
            else:
                pl.when(cond)(c.wait_send)


def own_event(gather):
    return gather.events()[0]


def gather_all(gathers, then=None):
    for g in gathers:
        if not g.sent:
            g.forward(own_event(g))
    for steps in zip(*[g.events()[1:] for g in gathers]):
        for i, (g, event) in enumerate(zip(gathers, steps)):
            g.arrive(event)
            g.forward(event)
            if then is not None:
                then(i, g.block(event))
    for g in gathers:
        g.drain()


class Scatter:
    def __init__(self, me, part, bufs, stage, order, send_sem, recv_sem):
        self.me, self.part, self.bufs, self.stage = me, part, bufs, stage
        self.order, self.send_sem, self.recv_sem = order, send_sem, recv_sem
        self.sent = []

    def slot(self, js):
        return flat(self.order, js)

    def copy(self, js):
        axis = next(i for i, j in enumerate(js) if j)
        slot = self.slot(js)
        peer = shifted(self.me, self.order, tuple(j if i == axis else 0 for i, j in enumerate(js)), 1)
        src = self.part.at[shifted(self.me, self.order, js, 1)] if axis == 0 else self.stage.at[slot]
        return pltpu.make_async_remote_copy(
            src_ref=src,
            dst_ref=self.bufs.at[slot],
            send_sem=self.send_sem.at[slot],
            recv_sem=self.recv_sem.at[slot],
            device_id={"fs": peer},
            device_id_type=pl.DeviceIdType.MESH,
        )

    def summed(self, js):
        axis = next((i for i, j in enumerate(js) if j), len(js))
        total = self.part[shifted(self.me, self.order, js, 1)]
        for i in range(axis):
            for off in range(1, self.order[i][0]):
                src = tuple(off if k == i else (js[k] if k > i else 0) for k in range(len(js)))
                self.copy(src).wait_recv()
                total = total + self.bufs[self.slot(src)]
        return total

    def tasks(self):
        rows = list(itertools.product(*[range(s) for s, _ in self.order]))
        first = lambda js: next((i for i, j in enumerate(js) if j), len(js))
        return sorted(rows, key=lambda js: (first(js), first(js[first(js) + 1:]) if first(js) < len(js) else 0))

    def run(self, js):
        if not any(js):
            return
        axis = next(i for i, j in enumerate(js) if j)
        if axis > 0:
            self.stage[self.slot(js)] = self.summed(js)
        c = self.copy(js)
        c.start()
        self.sent.append(c)

    def drain(self):
        for c in self.sent:
            c.wait_send()


def two_parts(wide):
    upper = wide.astype(jnp.bfloat16)
    lower = (wide - upper.astype(jnp.float32)).astype(jnp.bfloat16)
    return upper, lower


def dot(a, b, dims=(((1,), (0,)), ((), ()))):
    return lax.dot_general(a, b, dims, preferred_element_type=jnp.float32)


def merged(ref):
    n, r, c = ref.shape
    if r % 8 == 0:
        return ref[...].reshape(n * r, c)
    return jnp.concatenate([ref[i] for i in range(n)], axis=0)


def merged_halves(ref):
    n, h, r, c = ref.shape
    if r % 16 == 0:
        return ref[...].reshape(n * h * r, c)
    return jnp.concatenate([ref[i, j] for i in range(n) for j in range(h)], axis=0)


def kernel(
    n, m, total_size,
    x_hbm, vc_hbm, mo_hbm, oc_hbm, vw_hbm, ow_hbm, vf_hbm, vs_hbm, of_hbm, os_hbm, vb, ob,
    vnew, onew, vstep, ostep, vcopy, ocopy, vf_new, vs_new, of_new, os_new,
    x_ref, vc_ref, mo_ref, oc_ref, vw, ow, vf, vs, of, os_,
    vb_all, ob_all, vpart, opart, vacc, oacc, vrs, ors, vstage, ostage, vdir, odir, squares,
    load_sem, g_send, g_recv, s_send, s_recv, q_send, q_recv, p_send, p_recv,
):
    me = lax.axis_index("fs")
    mine = lax.axis_index("tp")
    digits = split_digits(n)
    order_a, order_b = orders_of(digits)

    pairs = (
        (mo_hbm, mo_ref), (oc_hbm, oc_ref), (x_hbm, x_ref), (vc_hbm, vc_ref),
        (vf_hbm, vf), (vs_hbm, vs), (of_hbm, of), (os_hbm, os_), (vw_hbm, vw), (ow_hbm, ow),
    )
    loads = [pltpu.make_async_copy(src, dst, load_sem.at[i]) for i, (src, dst) in enumerate(pairs)]

    barrier = pltpu.get_barrier_semaphore()
    peers = 0
    for size, stride in digits:
        for off in range(1, size):
            pl.semaphore_signal(
                barrier, inc=1, device_id={"fs": shifted(me, [(size, stride)], (off,), 1)},
                device_id_type=pl.DeviceIdType.MESH,
            )
            peers += 1
    for off in range(1, m):
        pl.semaphore_signal(
            barrier, inc=1, device_id={"tp": lax.rem(mine + off, m)},
            device_id_type=pl.DeviceIdType.MESH,
        )
        peers += 1
    for c in loads:
        c.start()
    halves = vb_all.shape[1]
    for whole, held in ((vb, vb_all), (ob, ob_all)):
        rows = held.shape[2]
        for h in range(halves):
            held[me, h] = whole[h * rows:(h + 1) * rows, :]
    pl.semaphore_wait(barrier, peers)

    half = lax.rem(mine, halves)
    sibling = mine + 1 - 2 * half
    bases = (vb_all, ob_all)

    def hand(i, block, part):
        return pltpu.make_async_remote_copy(
            src_ref=bases[i].at[block, part], dst_ref=bases[i].at[block, part],
            send_sem=p_send.at[i, block], recv_sem=p_recv.at[i, block],
            device_id={"tp": sibling}, device_id_type=pl.DeviceIdType.MESH,
        )

    handed = []

    def share(i, block):
        if halves == 2:
            c = hand(i, block, half)
            c.start()
            handed.append((i, block, c))

    gather_all([
        Gather(me, lambda b: vb_all.at[b, half], order_a, g_send.at[0], g_recv.at[0]),
        Gather(me, lambda b: ob_all.at[b, half], order_b, g_send.at[1], g_recv.at[1]),
    ], share)
    for i, block, c in handed:
        c.wait_send()
        hand(i, block, 1 - half).wait_recv()

    tokens = x_ref.shape[0]
    tile = min(256, tokens)
    r = vpart.shape[1]

    def project(src, cot, basis, acc, part):
        acc[...] = jnp.zeros_like(acc)

        def body(t, carry):
            rows = pl.ds(pl.multiple_of(t * tile, tile), tile)
            upper, lower = two_parts(dot(src[rows, :], basis))
            dims = (((0,), (0,)), ((), ()))
            cots = cot[rows, :]
            acc[...] += dot(upper, cots, dims) + dot(lower, cots, dims)
            return carry
        lax.fori_loop(0, tokens // tile, body, 0)
        for i in range(n):
            part[i] = acc[i * r:(i + 1) * r, :]

    scatter_v = Scatter(me, vpart, vrs, vstage, order_a[::-1], s_send.at[0], s_recv.at[0])
    scatter_o = Scatter(me, opart, ors, ostage, order_b[::-1], s_send.at[1], s_recv.at[1])
    loads[0].wait()
    loads[1].wait()
    project(mo_ref, oc_ref, merged_halves(ob_all), oacc, opart)
    tasks_o = scatter_o.tasks()
    early = [js for js in tasks_o if js[0]]
    for js in early:
        scatter_o.run(js)
    loads[2].wait()
    loads[3].wait()
    project(x_ref, vc_ref, merged_halves(vb_all), vacc, vpart)
    tasks_v = scatter_v.tasks()
    for js in tasks_v[:len(early)]:
        scatter_v.run(js)
    for js_o, js_v in zip(tasks_o[len(early):], tasks_v[len(early):]):
        scatter_o.run(js_o)
        scatter_v.run(js_v)
    for c in loads[4:]:
        c.wait()

    def moments(projected, first, second, first_new, second_new):
        fn = first_decay * first[...] + (1.0 - first_decay) * projected
        sn = second_decay * second[...] + (1.0 - second_decay) * projected * projected
        first_new[...] = fn
        second_new[...] = sn
        return fn / jnp.sqrt(sn)

    zero = (0,) * len(digits)
    gathers = [
        Gather(me, lambda b: odir.at[b], order_b, g_send.at[1], g_recv.at[3]),
        Gather(me, lambda b: vdir.at[b], order_a, g_send.at[0], g_recv.at[2]),
    ]
    odir[me] = moments(scatter_o.summed(zero), of, os_, of_new, os_new)
    gathers[0].forward(own_event(gathers[0]))
    vdir[me] = moments(scatter_v.summed(zero), vf, vs, vf_new, vs_new)
    gathers[1].forward(own_event(gathers[1]))
    scatter_o.drain()
    scatter_v.drain()
    gather_all(gathers)
    v_dir = merged(vdir)
    o_dir = merged(odir)
    squares[0] = jnp.full(squares.shape[1:], jnp.sum(v_dir * v_dir) + jnp.sum(o_dir * o_dir), jnp.float32)
    traded = []
    for off in range(1, m):
        c = pltpu.make_async_remote_copy(
            src_ref=squares.at[0], dst_ref=squares.at[off],
            send_sem=q_send.at[off], recv_sem=q_recv.at[off],
            device_id={"tp": lax.rem(mine + off, m)}, device_id_type=pl.DeviceIdType.MESH,
        )
        c.start()
        traded.append(c)
    v_upper, v_lower = two_parts(v_dir)
    o_upper, o_lower = two_parts(o_dir)
    v_sum = dot(vb[...], v_upper) + dot(vb[...], v_lower)
    o_sum = dot(ob[...], o_upper) + dot(ob[...], o_lower)
    for c in traded:
        c.wait()
    total = squares[0]
    for off in range(1, m):
        total = total + squares[off]
    scale = (step_rate / jnp.sqrt(1.0 + total / total_size))[0:1, 0:1]

    def update(weight, product, new, step, copy):
        s = scale * product
        w = weight[...] - s
        step[...] = s
        new[...] = w
        copy[me] = w.astype(jnp.bfloat16)

    gathers = [
        Gather(me, lambda b: vcopy.at[b], order_a, g_send.at[0], g_recv.at[4]),
        Gather(me, lambda b: ocopy.at[b], order_b, g_send.at[1], g_recv.at[5]),
    ]
    update(vw, v_sum, vnew, vstep, vcopy)
    gathers[0].forward(own_event(gathers[0]))
    update(ow, o_sum, onew, ostep, ocopy)
    gather_all(gathers)


def store(*refs):
    count = (len(refs) - 1) // 2
    ins, outs, sems = refs[:count], refs[count:2 * count], refs[-1]
    copies = [pltpu.make_async_copy(i, o, sems.at[k]) for k, (i, o) in enumerate(zip(ins, outs))]
    for c in copies:
        c.start()
    for c in copies:
        c.wait()


def local(n, m, x, vc, mo, oc, vw, ow, vb, ob, vf, vs, of, os_):
    f32, bf16 = jnp.float32, jnp.bfloat16
    r, v_cols = vf.shape
    o_cols = of.shape[1]
    total_size = float(n * r * m * (v_cols + o_cols))
    halves = 2 if m % 2 == 0 else 1
    vmem = pl.BlockSpec(memory_space=pltpu.VMEM)
    hbm = pl.BlockSpec(memory_space=pltpu.HBM)
    anywhere = pl.BlockSpec(memory_space=pl.ANY)
    outs = (
        (vw.shape, f32), (ow.shape, f32), (vw.shape, f32), (ow.shape, f32),
        ((n, *vw.shape), bf16), ((n, *ow.shape), bf16),
        (vf.shape, f32), (vf.shape, f32), (of.shape, f32), (of.shape, f32),
    )
    dma = pltpu.SemaphoreType.DMA
    big = (x, vc, mo, oc, vw, ow, vf, vs, of, os_)
    ways = 2 + sum(s - 1 for s, _ in split_digits(n)[:-1])
    res = pl.pallas_call(
        functools.partial(kernel, n, m, total_size),
        out_shape=tuple(pltpu.VMEM(s, d) for s, d in outs),
        in_specs=[hbm] * 10 + [vmem] * 2,
        out_specs=[vmem] * 10,
        scratch_shapes=[
            *[pltpu.VMEM(a.shape, a.dtype) for a in big],
            pltpu.VMEM((n, halves, vb.shape[0] // halves, vb.shape[1]), bf16),
            pltpu.VMEM((n, halves, ob.shape[0] // halves, ob.shape[1]), bf16),
            pltpu.VMEM((n, r, v_cols), f32), pltpu.VMEM((n, r, o_cols), f32),
            pltpu.VMEM((n * r, v_cols), f32), pltpu.VMEM((n * r, o_cols), f32),
            pltpu.VMEM((n, r, v_cols), f32), pltpu.VMEM((n, r, o_cols), f32),
            pltpu.VMEM((n, r, v_cols), f32), pltpu.VMEM((n, r, o_cols), f32),
            pltpu.VMEM((n, r, v_cols), f32), pltpu.VMEM((n, r, o_cols), f32),
            pltpu.VMEM((m, 8, 128), f32),
            dma((10,)), dma((2, n, ways)), dma((6, n)), dma((2, n)), dma((2, n)), dma((m,)), dma((m,)),
            dma((2, n)), dma((2, n)),
        ],
        compiler_params=pltpu.CompilerParams(
            collective_id=0, has_side_effects=True, vmem_limit_bytes=36 * 1024 * 1024
        ),
    )(*[pltpu.with_memory_space_constraint(a, pltpu.HBM) for a in big], vb, ob)
    res = pl.pallas_call(
        store,
        out_shape=tuple(jax.ShapeDtypeStruct(s, d) for s, d in outs),
        in_specs=[anywhere] * 10,
        out_specs=[hbm] * 10,
        scratch_shapes=[dma((10,))],
        compiler_params=pltpu.CompilerParams(vmem_limit_bytes=1024 * 1024),
    )(*res)
    vcopy, ocopy = res[4], res[5]
    return (
        *res[:4],
        vcopy.reshape(n * vw.shape[0], v_cols),
        ocopy.reshape(n * ow.shape[0], o_cols),
        *res[6:],
    )


def solution(mesh):
    n, m = mesh.shape["fs"], mesh.shape["tp"]
    rows, both, cols = P("fs", None), P("fs", "tp"), P(None, "tp")
    return jax.shard_map(
        functools.partial(local, n, m),
        mesh=mesh,
        in_specs=(rows, both, rows, both, both, both, rows, rows, both, both, both, both),
        out_specs=(both, both, both, both, cols, cols, both, both, both, both),
        check_vma=False,
    )
```

```python
import functools
import itertools

import jax
import jax.numpy as jnp
from jax import lax
from jax.experimental import pallas as pl
from jax.experimental.pallas import tpu as pltpu
from jax.sharding import PartitionSpec as P

first_decay = 0.8
second_decay = 0.9
step_rate = 0.1


def split_digits(n):
    digits = []
    stride = 1
    for _ in range(2):
        if n % 2 == 0 and n > 2:
            digits.append((2, stride))
            stride *= 2
            n //= 2
    digits.append((n, stride))
    return digits


def orders_of(digits):
    slow, fast = digits[-1], digits[:-1]
    back = fast[::-1]
    return [slow, *fast], [slow, *back], [fast[0], slow, *fast[1:]], [back[0], slow, *back[1:]]


def shifted(me, order, offsets, sign):
    out = me
    for (size, stride), off in zip(order, offsets):
        if off:
            digit = lax.rem(lax.div(me, stride), size)
            other = lax.rem(digit + (off if sign > 0 else size - off), size)
            out = out + (other - digit) * stride
    return out


def flat(order, offsets):
    out = 0
    for (size, _), off in zip(order, offsets):
        out = out * size + off
    return out


class Line:
    def __init__(self, me, digit):
        self.size, self.stride = digit
        self.me = me
        self.at = lax.div(me, self.stride)

    def nearest(self, t):
        if t == 0:
            return self.at
        k, z = self.size, self.at
        near = jnp.minimum(z, k - 1 - z)
        low = z < k - 1 - z
        step = (t + 1) // 2 if t % 2 else -(t // 2)
        both = jnp.where(low, z - step, z + step)
        one = jnp.where(low, z + (t - near), z - (t - near))
        return jnp.where(t <= 2 * near, both, one)


class Gather:
    def __init__(self, me, dst, order, slow, send_sem, recv_sem, line_sem=None):
        self.me, self.dst, self.order = me, dst, order
        self.slow = order.index(slow)
        self.line = Line(me, slow)
        self.send_sem, self.recv_sem, self.line_sem = send_sem, recv_sem, line_sem
        self.sent = []

    def events(self):
        rows = []
        last = len(self.order) - 1
        for at in itertools.product(*[range(s) for s, _ in self.order]):
            phase = max([i for i, j in enumerate(at) if j], default=-1)
            due = sum(j if i == self.slow else 1.25 * (j > 0) for i, j in enumerate(at))
            if phase == last and last != self.slow:
                due += 100
            rows.append((due, phase, at))
        return sorted(rows)

    def block(self, event):
        at = event[2]
        fast = [d for i, d in enumerate(self.order) if i != self.slow]
        offs = [j for i, j in enumerate(at) if i != self.slow]
        z = self.line.nearest(at[self.slow])
        return shifted(self.me, fast, offs, -1) + (z - self.line.at) * self.line.stride

    def copy(self, block, peer, send):
        return pltpu.make_async_remote_copy(
            src_ref=self.dst(block),
            dst_ref=self.dst(block),
            send_sem=send,
            recv_sem=self.recv_sem.at[block],
            device_id={"fs": peer},
            device_id_type=pl.DeviceIdType.MESH,
        )

    def start(self, cond, c):
        if cond is None:
            c.start()
        else:
            pl.when(cond)(c.start)
        self.sent.append((cond, c))

    def along_line(self, block, t):
        z, k, stride = self.line.at, self.line.size, self.line.stride
        if self.line_sem is not None:
            if t == 0:
                for other in range(1, k):
                    peer = self.me + (self.line.nearest(other) - z) * stride
                    self.start(None, self.copy(block, peer, self.line_sem.at[other]))
            return
        up = z + 1 < k
        down = z > 0
        if t > 0:
            source = self.line.nearest(t)
            up = jnp.logical_and(up, source < z)
            down = jnp.logical_and(down, source > z)
        base = lax.rem(self.me, stride)
        self.start(up, self.copy(block, jnp.minimum(self.me + stride, (k - 1) * stride + base), self.send_sem.at[block, 0]))
        self.start(down, self.copy(block, jnp.maximum(self.me - stride, base), self.send_sem.at[block, 1]))

    def forward(self, event):
        _, phase, at = event
        block = self.block(event)
        way = 2
        for axis, digit in enumerate(self.order):
            if axis == self.slow:
                if axis >= phase:
                    self.along_line(block, at[axis])
                continue
            for off in range(1, digit[0]):
                if axis > phase:
                    peer = shifted(self.me, [digit], (off,), 1)
                    self.start(None, self.copy(block, peer, self.send_sem.at[block, way]))
                way += 1

    def arrive(self, event):
        if any(event[2]):
            block = self.block(event)
            fast = self.order[0 if self.slow else 1]
            self.copy(block, shifted(self.me, [fast], (1,), 1), self.send_sem.at[block, 0]).wait_recv()

    def drain(self):
        for cond, c in self.sent:
            if cond is None:
                c.wait_send()
            else:
                pl.when(cond)(c.wait_send)


def own_event(gather):
    return gather.events()[0]


def gather_all(gathers, then=None):
    for g in gathers:
        if not g.sent:
            g.forward(own_event(g))
    for steps in zip(*[g.events()[1:] for g in gathers]):
        for i, (g, event) in enumerate(zip(gathers, steps)):
            g.arrive(event)
            g.forward(event)
            if then is not None:
                then(i, g.block(event))
    for g in gathers:
        g.drain()


class Scatter:
    def __init__(self, me, part, bufs, stage, cut, order, send_sem, recv_sem):
        self.me, self.part, self.bufs, self.stage, self.cut = me, part, bufs, stage, cut
        self.order, self.send_sem, self.recv_sem = order, send_sem, recv_sem
        self.sent = []

    def slot(self, js):
        return flat(self.order, js)

    def copy(self, js):
        axis = next(i for i, j in enumerate(js) if j)
        slot = self.slot(js)
        peer = shifted(self.me, self.order, tuple(j if i == axis else 0 for i, j in enumerate(js)), 1)
        src = self.part.at[shifted(self.me, self.order, js, 1), self.cut] if axis == 0 else self.stage.at[slot, self.cut]
        return pltpu.make_async_remote_copy(
            src_ref=src,
            dst_ref=self.bufs.at[slot, self.cut],
            send_sem=self.send_sem.at[slot],
            recv_sem=self.recv_sem.at[slot],
            device_id={"fs": peer},
            device_id_type=pl.DeviceIdType.MESH,
        )

    def summed(self, js):
        axis = next((i for i, j in enumerate(js) if j), len(js))
        total = self.part[shifted(self.me, self.order, js, 1), self.cut]
        for i in range(axis):
            for off in range(1, self.order[i][0]):
                src = tuple(off if k == i else (js[k] if k > i else 0) for k in range(len(js)))
                self.copy(src).wait_recv()
                total = total + self.bufs[self.slot(src), self.cut]
        return total

    def tasks(self):
        rows = list(itertools.product(*[range(s) for s, _ in self.order]))
        first = lambda js: next((i for i, j in enumerate(js) if j), len(js))
        return sorted(rows, key=lambda js: (first(js), first(js[first(js) + 1:]) if first(js) < len(js) else 0))

    def run(self, js):
        if not any(js):
            return
        axis = next(i for i, j in enumerate(js) if j)
        if axis > 0:
            self.stage[self.slot(js), self.cut] = self.summed(js)
        c = self.copy(js)
        c.start()
        self.sent.append(c)

    def drain(self):
        for c in self.sent:
            c.wait_send()


def two_parts(wide):
    upper = wide.astype(jnp.bfloat16)
    lower = (wide - upper.astype(jnp.float32)).astype(jnp.bfloat16)
    return upper, lower


def dot(a, b, dims=(((1,), (0,)), ((), ()))):
    return lax.dot_general(a, b, dims, preferred_element_type=jnp.float32)


def merged(ref):
    n, h, r, c = ref.shape
    if r % (32 // ref.dtype.itemsize) == 0:
        return ref[...].reshape(n * h * r, c)
    return jnp.concatenate([ref[i, j] for i in range(n) for j in range(h)], axis=0)


def kernel(
    n, m, total_size,
    x_hbm, vc_hbm, mo_hbm, oc_hbm, vw_hbm, ow_hbm, vf_hbm, vs_hbm, of_hbm, os_hbm, vb_hbm, ob_hbm,
    vnew, onew, vstep, ostep, vcopy, ocopy, vf_new, vs_new, of_new, os_new,
    x_ref, vc_ref, mo_ref, oc_ref, vw, ow, vf, vs, of, os_, vb, ob,
    vb_all, ob_all, vpart, opart, vacc, oacc, vrs, ors, vstage, ostage, vdir, odir, squares,
    load_sem, g_send, g_recv, s_send, s_recv, q_send, q_recv, p_send, p_recv, z_send,
):
    me = lax.axis_index("fs")
    mine = lax.axis_index("tp")
    digits = split_digits(n)
    order_a, order_b, order_c, order_d = orders_of(digits)
    slow = digits[-1]

    pairs = (
        (vb_hbm, vb), (ob_hbm, ob),
        (mo_hbm, mo_ref), (oc_hbm, oc_ref), (x_hbm, x_ref), (vc_hbm, vc_ref),
        (vf_hbm, vf), (vs_hbm, vs), (of_hbm, of), (os_hbm, os_), (vw_hbm, vw), (ow_hbm, ow),
    )
    loads = [pltpu.make_async_copy(src, dst, load_sem.at[i]) for i, (src, dst) in enumerate(pairs)]

    barrier = pltpu.get_barrier_semaphore()
    peers = 0
    for size, stride in digits:
        for off in range(1, size):
            pl.semaphore_signal(
                barrier, inc=1, device_id={"fs": shifted(me, [(size, stride)], (off,), 1)},
                device_id_type=pl.DeviceIdType.MESH,
            )
            peers += 1
    for off in range(1, m):
        pl.semaphore_signal(
            barrier, inc=1, device_id={"tp": lax.rem(mine + off, m)},
            device_id_type=pl.DeviceIdType.MESH,
        )
        peers += 1
    for c in loads:
        c.start()
    halves = vb_all.shape[1]
    loads[0].wait()
    loads[1].wait()
    for whole, held in ((vb, vb_all), (ob, ob_all)):
        rows = held.shape[2]
        for h in range(halves):
            held[me, h] = whole[h * rows:(h + 1) * rows, :]
    pl.semaphore_wait(barrier, peers)

    half = lax.rem(mine, halves)
    sibling = mine + 1 - 2 * half
    bases = (vb_all, ob_all)

    def hand(i, block, part):
        return pltpu.make_async_remote_copy(
            src_ref=bases[i].at[block, part], dst_ref=bases[i].at[block, part],
            send_sem=p_send.at[i, block], recv_sem=p_recv.at[i, block],
            device_id={"tp": sibling}, device_id_type=pl.DeviceIdType.MESH,
        )

    handed = []

    def share(i, block):
        if halves == 2:
            c = hand(i, block, half)
            c.start()
            handed.append((i, block, c))

    gather_all([
        Gather(me, lambda b: vb_all.at[b, half], order_a, slow, g_send.at[0], g_recv.at[0], z_send.at[0]),
        Gather(me, lambda b: ob_all.at[b, half], order_b, slow, g_send.at[1], g_recv.at[1], z_send.at[1]),
    ], share)
    for i, block, c in handed:
        c.wait_send()
        hand(i, block, 1 - half).wait_recv()

    tokens = x_ref.shape[0]
    tile = min(256, tokens)
    cuts, r = vpart.shape[1:3]

    def project(src, cot, basis, acc, part):
        acc[...] = jnp.zeros_like(acc)

        def body(t, carry):
            rows = pl.ds(pl.multiple_of(t * tile, tile), tile)
            upper, lower = two_parts(dot(src[rows, :], basis))
            dims = (((0,), (0,)), ((), ()))
            cots = cot[rows, :]
            acc[...] += dot(upper, cots, dims) + dot(lower, cots, dims)
            return carry
        lax.fori_loop(0, tokens // tile, body, 0)
        for i in range(n):
            for h in range(cuts):
                part[i, h] = acc[(i * cuts + h) * r:(i * cuts + h + 1) * r, :]

    turns = ((order_a, order_b), (order_b, order_a))
    scatters_v = [
        Scatter(me, vpart, vrs, vstage, h, turns[0][h % 2][::-1], s_send.at[h], s_recv.at[h])
        for h in range(cuts)
    ]
    scatters_o = [
        Scatter(me, opart, ors, ostage, h, turns[1][h % 2][::-1], s_send.at[cuts + h], s_recv.at[cuts + h])
        for h in range(cuts)
    ]
    loads[2].wait()
    loads[3].wait()
    project(mo_ref, oc_ref, merged(ob_all), oacc, opart)
    def run(scatters, first):
        lists = [[js for js in sc.tasks() if bool(js[0]) == first] for sc in scatters]
        for steps in zip(*lists):
            for sc, js in zip(scatters, steps):
                sc.run(js)

    run(scatters_o, True)
    loads[4].wait()
    loads[5].wait()
    project(x_ref, vc_ref, merged(vb_all), vacc, vpart)
    run(scatters_v, True)
    run(scatters_o + scatters_v, False)
    for c in loads[6:]:
        c.wait()

    def moments(projected, h, first, second, first_new, second_new):
        rows = slice(h * r, (h + 1) * r)
        fn = first_decay * first[rows, :] + (1.0 - first_decay) * projected
        sn = second_decay * second[rows, :] + (1.0 - second_decay) * projected * projected
        first_new[rows, :] = fn
        second_new[rows, :] = sn
        return fn / jnp.sqrt(sn)

    zero = (0,) * len(digits)
    ways = ((order_a, order_d), (order_b, order_c))

    def both(v_dst, o_dst, base):
        def make(dst, h, order, i):
            return Gather(me, lambda b: dst.at[b, h], order, slow, g_send.at[i], g_recv.at[base + i])
        return (
            [make(o_dst, h, ways[1][h % 2], cuts + h) for h in range(cuts)],
            [make(v_dst, h, ways[0][h % 2], h) for h in range(cuts)],
        )

    gathers_o, gathers_v = both(vdir, odir, 2)
    for h in range(cuts):
        odir[me, h] = moments(scatters_o[h].summed(zero), h, of, os_, of_new, os_new)
        gathers_o[h].forward(own_event(gathers_o[h]))
    for h in range(cuts):
        vdir[me, h] = moments(scatters_v[h].summed(zero), h, vf, vs, vf_new, vs_new)
        gathers_v[h].forward(own_event(gathers_v[h]))
    for sc in scatters_o + scatters_v:
        sc.drain()
    gather_all(gathers_o + gathers_v)
    v_dir = merged(vdir)
    o_dir = merged(odir)
    squares[0] = jnp.full(squares.shape[1:], jnp.sum(v_dir * v_dir) + jnp.sum(o_dir * o_dir), jnp.float32)
    traded = []
    for off in range(1, m):
        c = pltpu.make_async_remote_copy(
            src_ref=squares.at[0], dst_ref=squares.at[off],
            send_sem=q_send.at[off], recv_sem=q_recv.at[off],
            device_id={"tp": lax.rem(mine + off, m)}, device_id_type=pl.DeviceIdType.MESH,
        )
        c.start()
        traded.append(c)
    v_upper, v_lower = two_parts(v_dir)
    o_upper, o_lower = two_parts(o_dir)
    v_sum = dot(vb[...], v_upper) + dot(vb[...], v_lower)
    o_sum = dot(ob[...], o_upper) + dot(ob[...], o_lower)
    for c in traded:
        c.wait()
    total = squares[0]
    for off in range(1, m):
        total = total + squares[off]
    scale = (step_rate / jnp.sqrt(1.0 + total / total_size))[0:1, 0:1]

    gathers_o, gathers_v = both(vcopy, ocopy, 2 + 2 * cuts)

    def update(weight, product, new, step, copy, gathers):
        s = scale * product
        w = weight[...] - s
        rows = copy.shape[2]
        narrow = w.astype(jnp.bfloat16)
        for h, g in enumerate(gathers):
            copy[me, h] = narrow[h * rows:(h + 1) * rows, :]
            g.forward(own_event(g))
        step[...] = s
        new[...] = w

    update(vw, v_sum, vnew, vstep, vcopy, gathers_v)
    update(ow, o_sum, onew, ostep, ocopy, gathers_o)
    gather_all(gathers_v + gathers_o)


def store(*refs):
    count = (len(refs) - 1) // 2
    ins, outs, sems = refs[:count], refs[count:2 * count], refs[-1]
    copies = [pltpu.make_async_copy(i, o, sems.at[k]) for k, (i, o) in enumerate(zip(ins, outs))]
    for c in copies:
        c.start()
    for c in copies:
        c.wait()


def local(n, m, x, vc, mo, oc, vw, ow, vb, ob, vf, vs, of, os_):
    f32, bf16 = jnp.float32, jnp.bfloat16
    r, v_cols = vf.shape
    o_cols = of.shape[1]
    total_size = float(n * r * m * (v_cols + o_cols))
    halves = 2 if m % 2 == 0 else 1
    cuts = 2
    vmem = pl.BlockSpec(memory_space=pltpu.VMEM)
    hbm = pl.BlockSpec(memory_space=pltpu.HBM)
    anywhere = pl.BlockSpec(memory_space=pl.ANY)
    outs = (
        (vw.shape, f32), (ow.shape, f32), (vw.shape, f32), (ow.shape, f32),
        ((n, cuts, vw.shape[0] // cuts, v_cols), bf16), ((n, cuts, ow.shape[0] // cuts, o_cols), bf16),
        (vf.shape, f32), (vf.shape, f32), (of.shape, f32), (of.shape, f32),
    )
    dma = pltpu.SemaphoreType.DMA
    big = (x, vc, mo, oc, vw, ow, vf, vs, of, os_, vb, ob)
    ways = 2 + sum(s - 1 for s, _ in split_digits(n)[:-1])
    res = pl.pallas_call(
        functools.partial(kernel, n, m, total_size),
        out_shape=tuple(pltpu.VMEM(s, d) for s, d in outs),
        in_specs=[hbm] * 12,
        out_specs=[vmem] * 10,
        scratch_shapes=[
            *[pltpu.VMEM(a.shape, a.dtype) for a in big],
            pltpu.VMEM((n, halves, vb.shape[0] // halves, vb.shape[1]), bf16),
            pltpu.VMEM((n, halves, ob.shape[0] // halves, ob.shape[1]), bf16),
            pltpu.VMEM((n, cuts, r // cuts, v_cols), f32), pltpu.VMEM((n, cuts, r // cuts, o_cols), f32),
            pltpu.VMEM((n * r, v_cols), f32), pltpu.VMEM((n * r, o_cols), f32),
            pltpu.VMEM((n, cuts, r // cuts, v_cols), f32), pltpu.VMEM((n, cuts, r // cuts, o_cols), f32),
            pltpu.VMEM((n, cuts, r // cuts, v_cols), f32), pltpu.VMEM((n, cuts, r // cuts, o_cols), f32),
            pltpu.VMEM((n, cuts, r // cuts, v_cols), f32), pltpu.VMEM((n, cuts, r // cuts, o_cols), f32),
            pltpu.VMEM((m, 8, 128), f32),
            dma((12,)), dma((2 * cuts, n, ways)), dma((2 + 4 * cuts, n)), dma((2 * cuts, n)), dma((2 * cuts, n)),
            dma((m,)), dma((m,)), dma((2, n)), dma((2, n)), dma((2, split_digits(n)[-1][0])),
        ],
        compiler_params=pltpu.CompilerParams(
            collective_id=0, has_side_effects=True, vmem_limit_bytes=36 * 1024 * 1024
        ),
    )(*[pltpu.with_memory_space_constraint(a, pltpu.HBM) for a in big])
    res = pl.pallas_call(
        store,
        out_shape=tuple(jax.ShapeDtypeStruct(s, d) for s, d in outs),
        in_specs=[anywhere] * 10,
        out_specs=[hbm] * 10,
        scratch_shapes=[dma((10,))],
        compiler_params=pltpu.CompilerParams(vmem_limit_bytes=1024 * 1024),
    )(*res)
    vcopy, ocopy = res[4], res[5]
    return (
        *res[:4],
        vcopy.reshape(n * vw.shape[0], v_cols),
        ocopy.reshape(n * ow.shape[0], o_cols),
        *res[6:],
    )


def solution(mesh):
    n, m = mesh.shape["fs"], mesh.shape["tp"]
    rows, both, cols = P("fs", None), P("fs", "tp"), P(None, "tp")
    return jax.shard_map(
        functools.partial(local, n, m),
        mesh=mesh,
        in_specs=(rows, both, rows, both, both, both, rows, rows, both, both, both, both),
        out_specs=(both, both, both, both, cols, cols, both, both, both, both),
        check_vma=False,
    )
```

```python
import functools
import itertools

import jax
import jax.numpy as jnp
from jax import lax
from jax.experimental import pallas as pl
from jax.experimental.pallas import tpu as pltpu
from jax.sharding import PartitionSpec as P

first_decay = 0.8
second_decay = 0.9
step_rate = 0.1


def split_digits(n):
    digits = []
    stride = 1
    for _ in range(2):
        if n % 2 == 0 and n > 2:
            digits.append((2, stride))
            stride *= 2
            n //= 2
    digits.append((n, stride))
    return digits


def orders_of(digits):
    slow, fast = digits[-1], digits[:-1]
    back = fast[::-1]
    return [slow, *fast], [slow, *back], [fast[0], slow, *fast[1:]], [back[0], slow, *back[1:]]


def shifted(me, order, offsets, sign):
    out = me
    for (size, stride), off in zip(order, offsets):
        if off:
            digit = lax.rem(lax.div(me, stride), size)
            other = lax.rem(digit + (off if sign > 0 else size - off), size)
            out = out + (other - digit) * stride
    return out


def flat(order, offsets):
    out = 0
    for (size, _), off in zip(order, offsets):
        out = out * size + off
    return out


class Line:
    def __init__(self, me, digit):
        self.size, self.stride = digit
        self.me = me
        self.at = lax.div(me, self.stride)

    def nearest(self, t):
        if t == 0:
            return self.at
        k, z = self.size, self.at
        near = jnp.minimum(z, k - 1 - z)
        low = z < k - 1 - z
        step = (t + 1) // 2 if t % 2 else -(t // 2)
        both = jnp.where(low, z - step, z + step)
        one = jnp.where(low, z + (t - near), z - (t - near))
        return jnp.where(t <= 2 * near, both, one)


class Gather:
    def __init__(self, me, dst, order, slow, send_sem, recv_sem, line_sem=None):
        self.me, self.dst, self.order = me, dst, order
        self.slow = order.index(slow)
        self.line = Line(me, slow)
        self.send_sem, self.recv_sem, self.line_sem = send_sem, recv_sem, line_sem
        self.sent = []

    def events(self):
        rows = []
        last = len(self.order) - 1
        for at in itertools.product(*[range(s) for s, _ in self.order]):
            phase = max([i for i, j in enumerate(at) if j], default=-1)
            due = sum(j if i == self.slow else 1.25 * (j > 0) for i, j in enumerate(at))
            if phase == last and last != self.slow:
                due += 100
            rows.append((due, phase, at))
        return sorted(rows)

    def block(self, event):
        at = event[2]
        fast = [d for i, d in enumerate(self.order) if i != self.slow]
        offs = [j for i, j in enumerate(at) if i != self.slow]
        z = self.line.nearest(at[self.slow])
        return shifted(self.me, fast, offs, -1) + (z - self.line.at) * self.line.stride

    def copy(self, block, peer, send):
        return pltpu.make_async_remote_copy(
            src_ref=self.dst(block),
            dst_ref=self.dst(block),
            send_sem=send,
            recv_sem=self.recv_sem.at[block],
            device_id={"fs": peer},
            device_id_type=pl.DeviceIdType.MESH,
        )

    def start(self, cond, c):
        if cond is None:
            c.start()
        else:
            pl.when(cond)(c.start)
        self.sent.append((cond, c))

    def along_line(self, block, t):
        z, k, stride = self.line.at, self.line.size, self.line.stride
        if self.line_sem is not None:
            if t == 0:
                for other in range(1, k):
                    peer = self.me + (self.line.nearest(other) - z) * stride
                    self.start(None, self.copy(block, peer, self.line_sem.at[other]))
            return
        up = z + 1 < k
        down = z > 0
        if t > 0:
            source = self.line.nearest(t)
            up = jnp.logical_and(up, source < z)
            down = jnp.logical_and(down, source > z)
        base = lax.rem(self.me, stride)
        self.start(up, self.copy(block, jnp.minimum(self.me + stride, (k - 1) * stride + base), self.send_sem.at[block, 0]))
        self.start(down, self.copy(block, jnp.maximum(self.me - stride, base), self.send_sem.at[block, 1]))

    def forward(self, event):
        _, phase, at = event
        block = self.block(event)
        way = 2
        for axis, digit in enumerate(self.order):
            if axis == self.slow:
                if axis >= phase:
                    self.along_line(block, at[axis])
                continue
            for off in range(1, digit[0]):
                if axis > phase:
                    peer = shifted(self.me, [digit], (off,), 1)
                    self.start(None, self.copy(block, peer, self.send_sem.at[block, way]))
                way += 1

    def arrive(self, event):
        if any(event[2]):
            block = self.block(event)
            fast = self.order[0 if self.slow else 1]
            self.copy(block, shifted(self.me, [fast], (1,), 1), self.send_sem.at[block, 0]).wait_recv()

    def drain(self):
        for cond, c in self.sent:
            if cond is None:
                c.wait_send()
            else:
                pl.when(cond)(c.wait_send)


def own_event(gather):
    return gather.events()[0]


def gather_all(gathers, then=None):
    for g in gathers:
        if not g.sent:
            g.forward(own_event(g))
    for steps in zip(*[g.events()[1:] for g in gathers]):
        for i, (g, event) in enumerate(zip(gathers, steps)):
            g.arrive(event)
            g.forward(event)
            if then is not None:
                then(i, g.block(event))
    for g in gathers:
        g.drain()


class Scatter:
    def __init__(self, me, part, bufs, stage, cut, order, send_sem, recv_sem):
        self.me, self.part, self.bufs, self.stage, self.cut = me, part, bufs, stage, cut
        self.order, self.send_sem, self.recv_sem = order, send_sem, recv_sem
        self.sent = []

    def slot(self, js):
        return flat(self.order, js)

    def copy(self, js):
        axis = next(i for i, j in enumerate(js) if j)
        slot = self.slot(js)
        peer = shifted(self.me, self.order, tuple(j if i == axis else 0 for i, j in enumerate(js)), 1)
        src = self.part.at[shifted(self.me, self.order, js, 1), self.cut] if axis == 0 else self.stage.at[slot, self.cut]
        return pltpu.make_async_remote_copy(
            src_ref=src,
            dst_ref=self.bufs.at[slot, self.cut],
            send_sem=self.send_sem.at[slot],
            recv_sem=self.recv_sem.at[slot],
            device_id={"fs": peer},
            device_id_type=pl.DeviceIdType.MESH,
        )

    def summed(self, js):
        axis = next((i for i, j in enumerate(js) if j), len(js))
        total = self.part[shifted(self.me, self.order, js, 1), self.cut]
        for i in range(axis):
            for off in range(1, self.order[i][0]):
                src = tuple(off if k == i else (js[k] if k > i else 0) for k in range(len(js)))
                self.copy(src).wait_recv()
                total = total + self.bufs[self.slot(src), self.cut]
        return total

    def tasks(self):
        rows = list(itertools.product(*[range(s) for s, _ in self.order]))
        first = lambda js: next((i for i, j in enumerate(js) if j), len(js))
        return sorted(rows, key=lambda js: (first(js), first(js[first(js) + 1:]) if first(js) < len(js) else 0))

    def run(self, js):
        if not any(js):
            return
        axis = next(i for i, j in enumerate(js) if j)
        if axis > 0:
            self.stage[self.slot(js), self.cut] = self.summed(js)
        c = self.copy(js)
        c.start()
        self.sent.append(c)

    def drain(self):
        for c in self.sent:
            c.wait_send()


def two_parts(wide):
    upper = wide.astype(jnp.bfloat16)
    lower = (wide - upper.astype(jnp.float32)).astype(jnp.bfloat16)
    return upper, lower


def dot(a, b, dims=(((1,), (0,)), ((), ()))):
    return lax.dot_general(a, b, dims, preferred_element_type=jnp.float32)


def merged(ref):
    n, h, r, c = ref.shape
    if r % (32 // ref.dtype.itemsize) == 0:
        return ref[...].reshape(n * h * r, c)
    return jnp.concatenate([ref[i, j] for i in range(n) for j in range(h)], axis=0)


def kernel(
    n, m, total_size,
    x_hbm, vc_hbm, mo_hbm, oc_hbm, vw_hbm, ow_hbm, vf_hbm, vs_hbm, of_hbm, os_hbm, vb_hbm, ob_hbm,
    vnew, onew, vstep, ostep, vcopy, ocopy, vf_new, vs_new, of_new, os_new,
    x_ref, vc_ref, mo_ref, oc_ref, vw, ow, vf, vs, of, os_, vb, ob,
    vb_all, ob_all, vpart, opart, vacc, oacc, vrs, ors, vstage, ostage, vdir, odir, squares,
    load_sem, g_send, g_recv, s_send, s_recv, q_send, q_recv, p_send, p_recv, z_send,
):
    me = lax.axis_index("fs")
    mine = lax.axis_index("tp")
    digits = split_digits(n)
    order_a, order_b, order_c, order_d = orders_of(digits)
    slow = digits[-1]

    pairs = (
        (vb_hbm, vb), (ob_hbm, ob),
        (mo_hbm, mo_ref), (oc_hbm, oc_ref), (x_hbm, x_ref), (vc_hbm, vc_ref),
        (vf_hbm, vf), (vs_hbm, vs), (of_hbm, of), (os_hbm, os_), (vw_hbm, vw), (ow_hbm, ow),
    )
    loads = [pltpu.make_async_copy(src, dst, load_sem.at[i]) for i, (src, dst) in enumerate(pairs)]

    barrier = pltpu.get_barrier_semaphore()
    peers = 0
    for size, stride in digits:
        for off in range(1, size):
            pl.semaphore_signal(
                barrier, inc=1, device_id={"fs": shifted(me, [(size, stride)], (off,), 1)},
                device_id_type=pl.DeviceIdType.MESH,
            )
            peers += 1
    for off in range(1, m):
        pl.semaphore_signal(
            barrier, inc=1, device_id={"tp": lax.rem(mine + off, m)},
            device_id_type=pl.DeviceIdType.MESH,
        )
        peers += 1
    for c in loads[:2]:
        c.start()
    halves = vb_all.shape[1]
    loads[0].wait()
    loads[1].wait()
    for whole, held in ((vb, vb_all), (ob, ob_all)):
        rows = held.shape[2]
        for h in range(halves):
            held[me, h] = whole[h * rows:(h + 1) * rows, :]
    pl.semaphore_wait(barrier, peers)

    half = lax.rem(mine, halves)
    sibling = mine + 1 - 2 * half
    bases = (vb_all, ob_all)

    def hand(i, block, part):
        return pltpu.make_async_remote_copy(
            src_ref=bases[i].at[block, part], dst_ref=bases[i].at[block, part],
            send_sem=p_send.at[i, block], recv_sem=p_recv.at[i, block],
            device_id={"tp": sibling}, device_id_type=pl.DeviceIdType.MESH,
        )

    handed = []

    def share(i, block):
        if halves == 2:
            c = hand(i, block, half)
            c.start()
            handed.append((i, block, c))

    gathers = [
        Gather(me, lambda b: vb_all.at[b, half], order_a, slow, g_send.at[0], g_recv.at[0], z_send.at[0]),
        Gather(me, lambda b: ob_all.at[b, half], order_b, slow, g_send.at[1], g_recv.at[1], z_send.at[1]),
    ]
    for g in gathers:
        g.forward(own_event(g))
    gather_all(gathers, share)
    for c in loads[2:]:
        c.start()
    for i, block, c in handed:
        c.wait_send()
        hand(i, block, 1 - half).wait_recv()

    tokens = x_ref.shape[0]
    tile = min(512, tokens)
    cuts, r = vpart.shape[1:3]

    def project(src, cot, basis, acc, part):
        acc[...] = jnp.zeros_like(acc)

        def body(t, carry):
            rows = pl.ds(pl.multiple_of(t * tile, tile), tile)
            upper, lower = two_parts(dot(src[rows, :], basis))
            dims = (((0,), (0,)), ((), ()))
            cots = cot[rows, :]
            acc[...] += dot(upper, cots, dims) + dot(lower, cots, dims)
            return carry
        lax.fori_loop(0, tokens // tile, body, 0)
        for i in range(n):
            for h in range(cuts):
                part[i, h] = acc[(i * cuts + h) * r:(i * cuts + h + 1) * r, :]

    turns = ((order_a, order_b), (order_b, order_a))
    scatters_v = [
        Scatter(me, vpart, vrs, vstage, h, turns[0][h % 2][::-1], s_send.at[h], s_recv.at[h])
        for h in range(cuts)
    ]
    scatters_o = [
        Scatter(me, opart, ors, ostage, h, turns[1][h % 2][::-1], s_send.at[cuts + h], s_recv.at[cuts + h])
        for h in range(cuts)
    ]
    loads[2].wait()
    loads[3].wait()
    project(mo_ref, oc_ref, merged(ob_all), oacc, opart)
    def run(scatters, first):
        lists = [[js for js in sc.tasks() if bool(js[0]) == first] for sc in scatters]
        for steps in zip(*lists):
            for sc, js in zip(scatters, steps):
                sc.run(js)

    run(scatters_o, True)
    loads[4].wait()
    loads[5].wait()
    project(x_ref, vc_ref, merged(vb_all), vacc, vpart)
    run(scatters_v, True)
    run(scatters_o + scatters_v, False)
    for c in loads[6:]:
        c.wait()

    def moments(projected, h, first, second, first_new, second_new):
        rows = slice(h * r, (h + 1) * r)
        fn = first_decay * first[rows, :] + (1.0 - first_decay) * projected
        sn = second_decay * second[rows, :] + (1.0 - second_decay) * projected * projected
        first_new[rows, :] = fn
        second_new[rows, :] = sn
        return fn / jnp.sqrt(sn)

    zero = (0,) * len(digits)
    ways = ((order_a, order_d), (order_b, order_c))

    def both(v_dst, o_dst, base):
        def make(dst, h, order, i):
            return Gather(me, lambda b: dst.at[b, h], order, slow, g_send.at[i], g_recv.at[base + i])
        return (
            [make(o_dst, h, ways[1][h % 2], cuts + h) for h in range(cuts)],
            [make(v_dst, h, ways[0][h % 2], h) for h in range(cuts)],
        )

    gathers_o, gathers_v = both(vdir, odir, 2)
    for h in range(cuts):
        odir[me, h] = moments(scatters_o[h].summed(zero), h, of, os_, of_new, os_new)
        gathers_o[h].forward(own_event(gathers_o[h]))
    for h in range(cuts):
        vdir[me, h] = moments(scatters_v[h].summed(zero), h, vf, vs, vf_new, vs_new)
        gathers_v[h].forward(own_event(gathers_v[h]))
    for sc in scatters_o + scatters_v:
        sc.drain()
    gather_all(gathers_o + gathers_v)
    v_dir = merged(vdir)
    o_dir = merged(odir)
    squares[0] = jnp.full(squares.shape[1:], jnp.sum(v_dir * v_dir) + jnp.sum(o_dir * o_dir), jnp.float32)
    traded = []
    for off in range(1, m):
        c = pltpu.make_async_remote_copy(
            src_ref=squares.at[0], dst_ref=squares.at[off],
            send_sem=q_send.at[off], recv_sem=q_recv.at[off],
            device_id={"tp": lax.rem(mine + off, m)}, device_id_type=pl.DeviceIdType.MESH,
        )
        c.start()
        traded.append(c)
    v_upper, v_lower = two_parts(v_dir)
    o_upper, o_lower = two_parts(o_dir)
    v_sum = dot(vb[...], v_upper) + dot(vb[...], v_lower)
    o_sum = dot(ob[...], o_upper) + dot(ob[...], o_lower)
    for c in traded:
        c.wait()
    total = squares[0]
    for off in range(1, m):
        total = total + squares[off]
    scale = (step_rate / jnp.sqrt(1.0 + total / total_size))[0:1, 0:1]

    gathers_o, gathers_v = both(vcopy, ocopy, 2 + 2 * cuts)

    def update(weight, product, new, step, copy, gathers):
        s = scale * product
        w = weight[...] - s
        rows = copy.shape[2]
        narrow = w.astype(jnp.bfloat16)
        for h, g in enumerate(gathers):
            copy[me, h] = narrow[h * rows:(h + 1) * rows, :]
            g.forward(own_event(g))
        step[...] = s
        new[...] = w

    update(vw, v_sum, vnew, vstep, vcopy, gathers_v)
    update(ow, o_sum, onew, ostep, ocopy, gathers_o)
    gather_all(gathers_v + gathers_o)


def store(*refs):
    count = (len(refs) - 1) // 2
    ins, outs, sems = refs[:count], refs[count:2 * count], refs[-1]
    copies = [pltpu.make_async_copy(i, o, sems.at[k]) for k, (i, o) in enumerate(zip(ins, outs))]
    for c in copies:
        c.start()
    for c in copies:
        c.wait()


def local(n, m, x, vc, mo, oc, vw, ow, vb, ob, vf, vs, of, os_):
    f32, bf16 = jnp.float32, jnp.bfloat16
    r, v_cols = vf.shape
    o_cols = of.shape[1]
    total_size = float(n * r * m * (v_cols + o_cols))
    halves = 2 if m % 2 == 0 else 1
    cuts = 2
    vmem = pl.BlockSpec(memory_space=pltpu.VMEM)
    hbm = pl.BlockSpec(memory_space=pltpu.HBM)
    anywhere = pl.BlockSpec(memory_space=pl.ANY)
    outs = (
        (vw.shape, f32), (ow.shape, f32), (vw.shape, f32), (ow.shape, f32),
        ((n, cuts, vw.shape[0] // cuts, v_cols), bf16), ((n, cuts, ow.shape[0] // cuts, o_cols), bf16),
        (vf.shape, f32), (vf.shape, f32), (of.shape, f32), (of.shape, f32),
    )
    dma = pltpu.SemaphoreType.DMA
    big = (x, vc, mo, oc, vw, ow, vf, vs, of, os_, vb, ob)
    ways = 2 + sum(s - 1 for s, _ in split_digits(n)[:-1])
    res = pl.pallas_call(
        functools.partial(kernel, n, m, total_size),
        out_shape=tuple(pltpu.VMEM(s, d) for s, d in outs),
        in_specs=[hbm] * 12,
        out_specs=[vmem] * 10,
        scratch_shapes=[
            *[pltpu.VMEM(a.shape, a.dtype) for a in big],
            pltpu.VMEM((n, halves, vb.shape[0] // halves, vb.shape[1]), bf16),
            pltpu.VMEM((n, halves, ob.shape[0] // halves, ob.shape[1]), bf16),
            pltpu.VMEM((n, cuts, r // cuts, v_cols), f32), pltpu.VMEM((n, cuts, r // cuts, o_cols), f32),
            pltpu.VMEM((n * r, v_cols), f32), pltpu.VMEM((n * r, o_cols), f32),
            pltpu.VMEM((n, cuts, r // cuts, v_cols), f32), pltpu.VMEM((n, cuts, r // cuts, o_cols), f32),
            pltpu.VMEM((n, cuts, r // cuts, v_cols), f32), pltpu.VMEM((n, cuts, r // cuts, o_cols), f32),
            pltpu.VMEM((n, cuts, r // cuts, v_cols), f32), pltpu.VMEM((n, cuts, r // cuts, o_cols), f32),
            pltpu.VMEM((m, 8, 128), f32),
            dma((12,)), dma((2 * cuts, n, ways)), dma((2 + 4 * cuts, n)), dma((2 * cuts, n)), dma((2 * cuts, n)),
            dma((m,)), dma((m,)), dma((2, n)), dma((2, n)), dma((2, split_digits(n)[-1][0])),
        ],
        compiler_params=pltpu.CompilerParams(
            collective_id=0, has_side_effects=True, vmem_limit_bytes=36 * 1024 * 1024
        ),
    )(*[pltpu.with_memory_space_constraint(a, pltpu.HBM) for a in big])
    res = pl.pallas_call(
        store,
        out_shape=tuple(jax.ShapeDtypeStruct(s, d) for s, d in outs),
        in_specs=[anywhere] * 10,
        out_specs=[hbm] * 10,
        scratch_shapes=[dma((10,))],
        compiler_params=pltpu.CompilerParams(vmem_limit_bytes=1024 * 1024),
    )(*res)
    vcopy, ocopy = res[4], res[5]
    return (
        *res[:4],
        vcopy.reshape(n * vw.shape[0], v_cols),
        ocopy.reshape(n * ow.shape[0], o_cols),
        *res[6:],
    )


def solution(mesh):
    n, m = mesh.shape["fs"], mesh.shape["tp"]
    rows, both, cols = P("fs", None), P("fs", "tp"), P(None, "tp")
    return jax.shard_map(
        functools.partial(local, n, m),
        mesh=mesh,
        in_specs=(rows, both, rows, both, both, both, rows, rows, both, both, both, both),
        out_specs=(both, both, both, both, cols, cols, both, both, both, both),
        check_vma=False,
    )
```
